32 devices in a mesh: ep: 8 (over z, y), tp: 4 (over x, core).
Axes of the slice: x: 2, y: 2, z: 4, core: 2. Of those that a mesh axis runs over, the one named last changes fastest.
Arguments:
- queries: bfloat16 [16384, 1024], P('ep', 'tp'), may hold values from -6 to 6
- keys_values: bfloat16 [16384, 512], P('ep', 'tp'), may hold values from -6 to 6
- sink_logits: float32 [16], replicated, may hold values from 4 to 8
- out_weight: bfloat16 [1024, 2048], replicated, may hold values from -4 to 4
- expert_tokens: bfloat16 [8192, 2048], P(('ep', 'tp')), may hold values from -6 to 6
- norm_gain: float32 [2048], replicated, may hold values from 0.1 to 1.9
- routes: int32 [8192, 2], P(('ep', 'tp')), may hold values from 0 to 7, all different within a row; in each aligned block of 256 rows (0 to 255, 256 to 511, ...) at most 96 rows name the same one
- route_weights: float32 [8192, 2], P(('ep', 'tp')), may hold values from 0.1 to 1
- gate_weight: bfloat16 [8, 2048, 1024], P('ep', None, 'tp'), may hold values from -0.125 to 0.125
- up_weight: bfloat16 [8, 2048, 1024], P('ep', None, 'tp'), may hold values from -0.125 to 0.125
- down_weight: bfloat16 [8, 1024, 2048], P('ep', 'tp'), may hold values from -0.1875 to 0.1875
Outputs:
- mixer_out: bfloat16 [16384, 2048], P(('ep', 'tp'))
- expert_out: bfloat16 [8192, 2048], P(('ep', 'tp'))
The draws below stay inside these ranges and needn't reach their ends.
Inputs may be any that keep to these rules, and one draw needn't show every extreme that they name: `routes`: each row names 2 different experts. In each aligned block of 256 rows, no expert is named by more than 96 rows, and in some block an expert is named by exactly 96 rows.
All inputs are finite; a program needn't handle non-finite values.
Results may differ from the reference program's by a relative error of at most 0.012.
Values may be sent and summed in bfloat16 or wider, within the bound.
A program may use at most 128 MiB of HBM per device.

```python
import math
import jax
import jax.numpy as jnp
import numpy as np
from jax import lax

D = 2048
HEADS = 16
KV_HEADS = 4
GROUP = 4
HEAD_DIM = 64
WINDOW = 128
FE = 1024
TOPK = 2
MOE_ROWS = 256
SEQ = 16384
MOE_TOKENS = 8192
EXPERTS = 8
CAP = 96
N_TP = 4


def draw_queries(key, part):
    noise_key = jax.random.fold_in(key, 11)
    return jax.random.truncated_normal(noise_key, -6.0, 6.0, (SEQ, HEADS * HEAD_DIM)).astype(jnp.bfloat16)


def draw_keys_values(key, part):
    noise_key = jax.random.fold_in(key, 17)
    return jax.random.truncated_normal(noise_key, -6.0, 6.0, (SEQ, KV_HEADS * 2 * HEAD_DIM)).astype(jnp.bfloat16)


def block_scale(key, shape, split, least, high):
    level = 1.0
    for axis_at, shards_of in split:
        draws = jax.random.uniform(jax.random.fold_in(jax.random.fold_in(key, 6), axis_at), (shards_of,), jnp.float32, least / len(split), high / len(split))
        level = level * jnp.repeat(jnp.exp(draws), shape[axis_at] // shards_of).reshape((-1,) + (1,) * (len(shape) - 1 - axis_at))
    return level


def routed_block(own_key, own, number, rows, number_of, top, most, lean):
    order = jax.random.permutation(own_key, number_of)
    crowded, usual = portions_of(number_of, rows * top, most, lean, True), portions_of(number_of, rows * top, most, lean, False)
    places = jnp.arange(number_of)

    def named(lengths, rotation):
        used = int((lengths > 0).sum())
        fixed = max(1, used // 4)
        moved = fixed + (places - fixed + rotation * (used - fixed)) % max(1, number_of - fixed)
        return jnp.zeros((number_of,), jnp.int32).at[order[jnp.where(places < fixed, places, moved)]].set(jnp.asarray(lengths, jnp.int32))

    lengths = jnp.where(number % 4 == 0, named(crowded, number // 4), named(usual, number - number // 4 - 1))
    mixed = jax.random.permutation(jax.random.fold_in(own, 3), number_of)
    giver, taker = mixed[0:number_of // 2 * 2:2], mixed[1:number_of // 2 * 2:2]
    margin = jnp.minimum(lengths[giver] - 1, most - lengths[taker]) // 2
    margin = jnp.where((giver == order[0]) | (taker == order[0]) | (lengths[taker] == 0), 0, jnp.maximum(margin, 0))
    moved = jax.random.randint(jax.random.fold_in(own, 4), (number_of // 2,), 0, 1 << 20) % (margin + 1)
    lengths = lengths.at[giver].add(-moved).at[taker].add(moved)
    items = jnp.searchsorted(jnp.cumsum(lengths), jnp.arange(rows * top), side="right").astype(jnp.int32)
    table = items.reshape(top, rows).T
    table = table[jax.random.permutation(jax.random.fold_in(own, 1), rows)]
    rotation = jax.random.randint(jax.random.fold_in(own, 2), (rows, 1), 0, top)
    return jnp.take_along_axis(table, (jnp.arange(top)[None, :] + rotation) % top, axis=1)


def portions_of(number_of, total, most, skew, full):
    portions = [(1 << 20) // math.isqrt(grade ** skew) + 1 for grade in range(1, number_of + 1)]
    largest = most if full else min(most, max(-(-total // number_of), total * portions[0] // sum(portions)))
    least = 1 if total - largest >= number_of - 1 else 0
    counts, surplus = [largest] + [least] * (number_of - 1), total - largest - least * (number_of - 1)
    while surplus > 0:
        candidates = [i for i in range(1, number_of) if counts[i] < largest] or [i for i in range(1, number_of) if counts[i] < most]
        whole, left = sum([portions[i] for i in candidates]), surplus
        for i in candidates:
            addition = min(most - counts[i], max(1, left * portions[i] // whole), surplus)
            counts[i] = counts[i] + addition
            surplus = surplus - addition
    return np.array(counts)


def normal_values(rng, dims, width, limit, cuts=(), kind=jnp.bfloat16):
    result = width * jax.random.normal(rng, dims, jnp.float32)
    if cuts:
        result = result * block_scale(rng, dims, cuts, -0.22, 0.18)
    return jnp.clip(result, -limit, limit).astype(kind)


def setup_inputs(seed: int = 0) -> dict:
    keys = jax.random.split(jax.random.key(seed), 12)
    queries = draw_queries(jax.random.fold_in(keys[11], 71), 0)
    keys_values = draw_keys_values(jax.random.fold_in(keys[11], 71), 0)
    sink_logits = jnp.clip(jax.random.uniform(keys[2], (HEADS,), jnp.float32, 4.0, 8.0), 4.0, 8.0)
    out_weight = normal_values(keys[3], (HEADS * HEAD_DIM, D), 0.8, 4.0)
    expert_tokens = normal_values(keys[4], (MOE_TOKENS, D), 1.0, 6.0, ((0, 32),))
    norm_gain = jnp.clip(1.0 + 0.18 * jax.random.normal(keys[5], (D,), jnp.float32), 0.1, 1.9)
    routes_keys = jax.random.split(jax.random.fold_in(keys[6], 1), MOE_TOKENS // MOE_ROWS)
    routes_turns = jax.random.permutation(jax.random.fold_in(keys[6], 3), MOE_TOKENS // MOE_ROWS)
    routes = jax.vmap(lambda own, number: routed_block(jax.random.fold_in(keys[6], 2), own, number, MOE_ROWS, EXPERTS, TOPK, CAP, 2))(routes_keys, routes_turns).reshape((MOE_TOKENS, TOPK))
    route_weights = jnp.clip(0.1 + 0.9 * jax.random.uniform(keys[7], (MOE_TOKENS, TOPK), jnp.float32) ** block_scale(keys[7], (MOE_TOKENS, TOPK), ((0, 32),), -0.2, 0.2), 0.1, 1.0)
    gate_weight = normal_values(keys[8], (EXPERTS, D, FE), D ** -0.5, 0.125, ((0, 8), (2, 4)))
    up_weight = normal_values(keys[9], (EXPERTS, D, FE), D ** -0.5, 0.125, ((0, 8), (2, 4)))
    down_weight = normal_values(keys[10], (EXPERTS, FE, D), FE ** -0.5, 0.1875, ((0, 8), (1, 4)))
    return dict(queries=queries, keys_values=keys_values, sink_logits=sink_logits, out_weight=out_weight, expert_tokens=expert_tokens, norm_gain=norm_gain, routes=routes, route_weights=route_weights, gate_weight=gate_weight, up_weight=up_weight, down_weight=down_weight)


NEG_FILL = -1e+30

def attend_all(queries, keys_values, sink_logits):
    seq_total = queries.shape[0]
    block_rows = min(512, seq_total)
    key_span = block_rows + 2 * WINDOW
    query_all = queries.astype(jnp.float32).reshape(seq_total, KV_HEADS, GROUP, HEAD_DIM)
    pair_all = keys_values.astype(jnp.float32).reshape(seq_total, KV_HEADS, 2, HEAD_DIM)
    padded = jnp.pad(pair_all, ((WINDOW, WINDOW), (0, 0), (0, 0), (0, 0)))
    sink_grid = sink_logits.astype(jnp.float32).reshape(KV_HEADS, GROUP, 1, 1)

    def one_block(block_index):
        first_row = block_index * block_rows
        query_block = lax.dynamic_slice_in_dim(query_all, first_row, block_rows, 0)
        pair_block = lax.dynamic_slice_in_dim(padded, first_row, key_span, 0)
        scores = jnp.einsum('qhgd,khd->hgqk', query_block, pair_block[:, :, 0]) * HEAD_DIM ** (-0.5)
        query_pos = first_row + jnp.arange(block_rows, dtype=jnp.int32)
        key_pos = first_row - WINDOW + jnp.arange(key_span, dtype=jnp.int32)
        allowed = (jnp.abs(query_pos[:, None] - key_pos[None, :]) <= WINDOW) & (key_pos >= 0)[None, :] & (key_pos < seq_total)[None, :]
        scores = jnp.where(allowed, scores, NEG_FILL)
        top_score = jnp.maximum(lax.optimization_barrier(jnp.max(scores, -1, keepdims=True)), sink_grid)
        exp_scores = jnp.exp(scores - top_score)
        denominator = lax.optimization_barrier(jnp.sum(exp_scores, -1, keepdims=True)) + jnp.exp(sink_grid - top_score)
        attn_weights = lax.optimization_barrier((exp_scores / denominator).astype(jnp.bfloat16)).astype(jnp.float32)
        head_values = jnp.einsum('hgqk,khd->qhgd', attn_weights, pair_block[:, :, 1])
        return head_values.astype(jnp.bfloat16).reshape(block_rows, HEADS * HEAD_DIM)
    blocks = lax.map(one_block, jnp.arange(seq_total // block_rows, dtype=jnp.int32))
    return blocks.reshape(seq_total, HEADS * HEAD_DIM)

def reference(queries, keys_values, sink_logits, out_weight, expert_tokens, norm_gain, routes, route_weights, gate_weight, up_weight, down_weight):
    attended = attend_all(queries, keys_values, sink_logits)
    mixer_out = jnp.dot(attended, out_weight, preferred_element_type=jnp.float32).astype(jnp.bfloat16)
    token_total = expert_tokens.shape[0]
    block_count = token_total // MOE_ROWS
    rows_float = expert_tokens.astype(jnp.float32)
    centred = rows_float - lax.optimization_barrier(jnp.mean(rows_float, -1, keepdims=True))
    normed = (centred * lax.rsqrt(lax.optimization_barrier(jnp.mean(centred * centred, -1, keepdims=True)) + 1e-06) * norm_gain).astype(jnp.bfloat16)
    flat_routes = routes.reshape(block_count, MOE_ROWS * TOPK).astype(jnp.int32)
    one_hot = (flat_routes[:, :, None] == jnp.arange(EXPERTS, dtype=jnp.int32)[None, None, :]).astype(jnp.int32)
    slot_rank = lax.optimization_barrier(jnp.sum((jnp.cumsum(one_hot, 1) - 1) * one_hot, -1))
    block_ids = jnp.arange(block_count, dtype=jnp.int32)[:, None]
    expert_slot = (flat_routes * (block_count * CAP) + block_ids * CAP + slot_rank).reshape(-1)
    copy_token = (block_ids * MOE_ROWS + jnp.arange(MOE_ROWS * TOPK, dtype=jnp.int32)[None, :] // TOPK).reshape(-1)
    slot_table = jnp.full((EXPERTS * block_count * CAP,), token_total, jnp.int32).at[expert_slot].set(copy_token)
    slot_table = slot_table.reshape(EXPERTS, block_count * CAP)
    weight_table = jnp.zeros((EXPERTS * block_count * CAP,), jnp.float32).at[expert_slot].set(route_weights.reshape(-1))
    weight_table = weight_table.reshape(EXPERTS, block_count * CAP)
    quarter = FE // N_TP

    def add_expert(running, expert_index):
        token_index = slot_table[expert_index]
        chosen = jnp.take(normed, token_index, axis=0, mode='fill', fill_value=0)
        gate_value = jnp.dot(chosen, gate_weight[expert_index], preferred_element_type=jnp.float32)
        up_value = jnp.dot(chosen, up_weight[expert_index], preferred_element_type=jnp.float32)
        hidden = (jax.nn.silu(gate_value) * up_value).astype(jnp.bfloat16)
        hidden_parts = hidden.astype(jnp.float32).reshape(-1, N_TP, quarter)
        down_parts = down_weight[expert_index].astype(jnp.float32).reshape(N_TP, quarter, -1)
        partial_value = jnp.einsum('rqf,qfd->qrd', hidden_parts, down_parts)
        partial_value = lax.optimization_barrier(partial_value.astype(jnp.bfloat16)).astype(jnp.float32)
        copy_result = lax.optimization_barrier(jnp.sum(partial_value, 0)).astype(jnp.bfloat16)
        update = lax.optimization_barrier(copy_result).astype(jnp.float32) * weight_table[expert_index][:, None]
        return (running.at[token_index].add(update, mode='drop'), None)
    total_out, unused = lax.scan(add_expert, jnp.zeros((token_total, expert_tokens.shape[1]), jnp.float32), jnp.arange(EXPERTS, dtype=jnp.int32))
    expert_out = total_out.astype(jnp.bfloat16)
    return (mixer_out, expert_out)
```

```python
import functools

import jax
import jax.numpy as jnp
from jax import lax
from jax.experimental import pallas as pl
from jax.experimental.pallas import tpu as pltpu
from jax.sharding import PartitionSpec as P

HEAD_DIM = 64
WINDOW = 128
TOPK = 2
NEG_FILL = -1e30


def gathered_shards(cells, axis):
    count = lax.axis_size(axis)
    if count & (count - 1):
        return [cells] + [
            lax.ppermute(cells, axis, [(i, (i + k) % count) for i in range(count)])
            for k in range(1, count)
        ]
    shards = [cells]
    bit = count // 2
    while bit:
        perm = [(i, i ^ bit) for i in range(count)]
        shards = shards + [lax.ppermute(shard, axis, perm) for shard in shards]
        bit //= 2
    return shards


def attend_kernel(kv_heads, group, rows, seq_total, offset_ref, q_ref, kv_ref, vk_ref, sink_ref, out_ref):
    step = pl.program_id(0)
    span = rows + 2 * WINDOW
    first = offset_ref[0] + step * rows
    start = pl.multiple_of(step * rows, rows)
    row = lax.broadcasted_iota(jnp.int32, (rows, span), 0)
    column = lax.broadcasted_iota(jnp.int32, (rows, span), 1)
    key_pos = first - WINDOW + column
    allowed = (
        (column >= row) & (column <= row + 2 * WINDOW) & (key_pos >= 0) & (key_pos < seq_total)
    )
    lower = lax.broadcasted_iota(jnp.int32, (rows, 2 * HEAD_DIM), 1) < HEAD_DIM
    for kv_head in range(kv_heads):
        lanes = slice(kv_head * 2 * HEAD_DIM, (kv_head + 1) * 2 * HEAD_DIM)
        kv = kv_ref[pl.ds(start, span), lanes]
        vk = vk_ref[pl.ds(start, span), lanes]
        for pair in range(group // 2):
            head = kv_head * group + 2 * pair
            cols = slice(head * HEAD_DIM, (head + 2) * HEAD_DIM)
            q_pair = q_ref[:, cols] * jnp.bfloat16(HEAD_DIM ** -0.5)
            results = []
            for odd in range(2):
                q_one = jnp.where(lower != bool(odd), q_pair, jnp.zeros_like(q_pair))
                key_side, value_side = (vk, kv) if odd else (kv, vk)
                scores = lax.dot_general(
                    q_one, key_side, (((1,), (1,)), ((), ())), preferred_element_type=jnp.float32
                )
                scores = jnp.where(allowed, scores, NEG_FILL)
                sink = sink_ref[head + odd]
                top = jnp.maximum(jnp.max(scores, 1, keepdims=True), sink)
                expo = jnp.exp(scores - top)
                denom = jnp.sum(expo, 1, keepdims=True) + jnp.exp(sink - top)
                value = jnp.dot(
                    expo.astype(jnp.bfloat16), value_side, preferred_element_type=jnp.float32
                )
                results.append(value / denom)
            out_ref[:, cols] = jnp.where(lower, results[0], results[1]).astype(jnp.bfloat16)


def attend(queries, keys_values, before, after, sink_logits):
    row_count, width = queries.shape
    kv_local = keys_values.shape[1] // (2 * HEAD_DIM)
    heads = width // HEAD_DIM
    rows = 128
    padded = jnp.concatenate([before, keys_values, after], 0)
    halves = padded.reshape(padded.shape[0], kv_local, 2, HEAD_DIM)
    swapped = halves[:, :, ::-1].reshape(padded.shape)
    offset = (lax.axis_index("ep") * row_count).astype(jnp.int32).reshape(1)
    sink_local = lax.dynamic_slice_in_dim(sink_logits, lax.axis_index("tp") * heads, heads, 0)
    seq_total = row_count * lax.axis_size("ep")
    span = rows + 2 * WINDOW
    smem = pl.BlockSpec(memory_space=pltpu.SMEM)
    whole = pl.BlockSpec(padded.shape, lambda i: (0, 0))
    return pl.pallas_call(
        functools.partial(attend_kernel, kv_local, heads // kv_local, rows, seq_total),
        out_shape=jax.ShapeDtypeStruct(queries.shape, jnp.bfloat16),
        grid=(row_count // rows,),
        in_specs=[smem, pl.BlockSpec((rows, width), lambda i: (i, 0)), whole, whole, smem],
        out_specs=pl.BlockSpec((rows, width), lambda i: (i, 0)),
        cost_estimate=pl.CostEstimate(
            flops=8 * row_count * span * heads * HEAD_DIM,
            bytes_accessed=4 * row_count * width,
            transcendentals=row_count * span * heads,
        ),
        name="attend",
    )(offset, queries, padded, swapped, sink_local)


def dispatch_kernel(experts, capacity, token_ref, gain_ref, route_ref, out_ref, slot_ref, normed_ref):
    step = pl.program_id(0)
    count = token_ref.shape[0]

    @pl.when(step == 0)
    def first():
        rows = token_ref[...].astype(jnp.float32)
        centred = rows - jnp.mean(rows, -1, keepdims=True)
        scale = lax.rsqrt(jnp.mean(centred * centred, -1, keepdims=True) + 1e-06)
        normed_ref[...] = (centred * scale * gain_ref[...]).astype(jnp.bfloat16)
        expert = lax.broadcasted_iota(jnp.int32, (experts, count), 0)
        named = [expert == route_ref[k : k + 1, :] for k in range(TOPK)]
        member = functools.reduce(jnp.logical_or, named)
        earlier = lax.broadcasted_iota(jnp.int32, (count, count), 0) < lax.broadcasted_iota(
            jnp.int32, (count, count), 1
        )
        rank = jnp.dot(
            jnp.where(member, 1.0, 0.0).astype(jnp.bfloat16),
            jnp.where(earlier, 1.0, 0.0).astype(jnp.bfloat16),
            preferred_element_type=jnp.float32,
        ).astype(jnp.int32)
        place = expert * capacity + rank
        for k in range(TOPK):
            slot_ref[k : k + 1, :] = jnp.sum(jnp.where(named[k], place, 0), 0, keepdims=True)

    tile = out_ref.shape[0]
    slot = step * tile + lax.broadcasted_iota(jnp.int32, (tile, count), 0)
    hit = functools.reduce(
        jnp.logical_or, [slot == slot_ref[k : k + 1, :] for k in range(TOPK)]
    )
    out_ref[...] = jnp.dot(
        jnp.where(hit, 1.0, 0.0).astype(jnp.bfloat16),
        normed_ref[...],
        preferred_element_type=jnp.float32,
    ).astype(jnp.bfloat16)


def dispatched(tokens, gain, routes, experts, capacity):
    count, width = tokens.shape
    total = experts * capacity
    return pl.pallas_call(
        functools.partial(dispatch_kernel, experts, capacity),
        out_shape=(
            jax.ShapeDtypeStruct((total, width), jnp.bfloat16),
            jax.ShapeDtypeStruct((TOPK, count), jnp.int32),
        ),
        grid=(total // count,),
        in_specs=[
            pl.BlockSpec((count, width), lambda i: (0, 0)),
            pl.BlockSpec((1, width), lambda i: (0, 0)),
            pl.BlockSpec((TOPK, count), lambda i: (0, 0)),
        ],
        out_specs=(
            pl.BlockSpec((count, width), lambda i: (i, 0)),
            pl.BlockSpec((TOPK, count), lambda i: (0, 0)),
        ),
        scratch_shapes=[pltpu.VMEM((count, width), jnp.bfloat16)],
        cost_estimate=pl.CostEstimate(
            flops=2 * total * count * width, bytes_accessed=2 * (total + count) * width,
            transcendentals=count,
        ),
        name="dispatch",
    )(tokens, gain.reshape(1, width), routes.T)


def expert_kernel(shards, block, x_ref, *refs):
    weights = refs[: 3 * shards]
    out_ref, gate_s, up_s, down_s, hidden_s, sems = refs[3 * shards :]
    first = pl.program_id(0) == 0

    def copies(shard, kinds):
        part = slice(shard * block, (shard + 1) * block)
        places = (gate_s.at[:, part], up_s.at[:, part], down_s.at[part, :])
        return [
            pltpu.make_async_copy(
                weights[3 * shard + kind], places[kind], sems.at[3 * shard + kind]
            )
            for kind in kinds
        ]

    @pl.when(first)
    def start():
        for kinds in ((0, 1), (2,)):
            for shard in range(shards):
                for copy in copies(shard, kinds):
                    copy.start()

    for shard in range(shards):
        part = slice(shard * block, (shard + 1) * block)

        @pl.when(first)
        def arrive():
            for copy in copies(shard, (0, 1)):
                copy.wait()

        gate = jnp.dot(x_ref[...], gate_s[:, part], preferred_element_type=jnp.float32)
        up = jnp.dot(x_ref[...], up_s[:, part], preferred_element_type=jnp.float32)
        hidden_s[:, part] = (gate / (1.0 + jnp.exp(-gate)) * up).astype(jnp.bfloat16)

    @pl.when(first)
    def arrive_down():
        for shard in range(shards):
            copies(shard, (2,))[0].wait()

    out_ref[...] = jnp.dot(
        hidden_s[...], down_s[...], preferred_element_type=jnp.float32
    ).astype(jnp.bfloat16)


def expert_rows(rows, gates, ups, downs, tile):
    total, width = rows.shape
    shards = len(gates)
    block = gates[0].shape[1]
    hidden = shards * block
    weights = [w for group in zip(gates, ups, downs) for w in group]
    return pl.pallas_call(
        functools.partial(expert_kernel, shards, block),
        out_shape=jax.ShapeDtypeStruct(rows.shape, jnp.bfloat16),
        grid=(total // tile,),
        in_specs=[pl.BlockSpec((tile, width), lambda i: (i, 0))]
        + [pl.BlockSpec(memory_space=pl.ANY)] * len(weights),
        out_specs=pl.BlockSpec((tile, width), lambda i: (i, 0)),
        scratch_shapes=[
            pltpu.VMEM((width, hidden), jnp.bfloat16),
            pltpu.VMEM((width, hidden), jnp.bfloat16),
            pltpu.VMEM((hidden, width), jnp.bfloat16),
            pltpu.VMEM((tile, hidden), jnp.bfloat16),
            pltpu.SemaphoreType.DMA((3 * shards,)),
        ],
        compiler_params=pltpu.CompilerParams(vmem_limit_bytes=48 * 1024 * 1024),
        cost_estimate=pl.CostEstimate(
            flops=6 * total * width * hidden,
            bytes_accessed=6 * width * hidden + 4 * total * width,
            transcendentals=total * hidden,
        ),
        name="experts",
    )(rows, *weights)


def combine_kernel(slot_ref, weight_ref, rows_ref, out_ref, high_ref, low_ref):
    @pl.when(pl.program_id(0) == 0)
    def first():
        count, total = high_ref.shape
        slot = lax.broadcasted_iota(jnp.int32, (count, total), 1)
        mix = sum(
            jnp.where(slot == slot_ref[:, k : k + 1], weight_ref[:, k : k + 1], 0.0)
            for k in range(TOPK)
        )
        high = mix.astype(jnp.bfloat16)
        high_ref[...] = high
        low_ref[...] = (mix - high.astype(jnp.float32)).astype(jnp.bfloat16)

    rows = rows_ref[...]
    out_ref[...] = (
        jnp.dot(high_ref[...], rows, preferred_element_type=jnp.float32)
        + jnp.dot(low_ref[...], rows, preferred_element_type=jnp.float32)
    ).astype(jnp.bfloat16)


def combined(rows, slots, route_weights):
    total, width = rows.shape
    count = route_weights.shape[0]
    tile = width // 4
    return pl.pallas_call(
        combine_kernel,
        out_shape=jax.ShapeDtypeStruct((count, width), jnp.bfloat16),
        grid=(width // tile,),
        in_specs=[
            pl.BlockSpec((count, TOPK), lambda i: (0, 0)),
            pl.BlockSpec((count, TOPK), lambda i: (0, 0)),
            pl.BlockSpec((total, tile), lambda i: (0, i)),
        ],
        out_specs=pl.BlockSpec((count, tile), lambda i: (0, i)),
        scratch_shapes=[
            pltpu.VMEM((count, total), jnp.bfloat16),
            pltpu.VMEM((count, total), jnp.bfloat16),
        ],
        cost_estimate=pl.CostEstimate(
            flops=4 * total * count * width, bytes_accessed=2 * (total + count) * width,
            transcendentals=0,
        ),
        name="combine",
    )(slots.T, route_weights, rows)


def body(
    queries,
    keys_values,
    sink_logits,
    out_weight,
    expert_tokens,
    norm_gain,
    routes,
    route_weights,
    gate_weight,
    up_weight,
    down_weight,
):
    ep_count = lax.axis_size("ep")
    row_count, model_width = expert_tokens.shape
    capacity = 3 * row_count * TOPK // (2 * ep_count)
    ends = ep_count - 1
    before = lax.ppermute(keys_values[-WINDOW:], "ep", [(i, i + 1) for i in range(ends)])
    after = lax.ppermute(keys_values[:WINDOW], "ep", [(i + 1, i) for i in range(ends)])
    gates = gathered_shards(gate_weight[0], "tp")
    ups = gathered_shards(up_weight[0], "tp")
    downs = gathered_shards(down_weight[0], "tp")
    outgoing, slots = dispatched(expert_tokens, norm_gain, routes, ep_count, capacity)
    outgoing, before, after = lax.optimization_barrier((outgoing, before, after))
    arrived = lax.all_to_all(
        outgoing.reshape(ep_count, capacity, model_width), "ep", 0, 0, tiled=True
    )
    attended = attend(queries, keys_values, before, after, sink_logits)
    token_rows = lax.all_to_all(attended, "tp", split_axis=0, concat_axis=1, tiled=True)
    mixer_out = jnp.dot(token_rows, out_weight, preferred_element_type=jnp.float32).astype(
        jnp.bfloat16
    )
    results = expert_rows(
        arrived.reshape(ep_count * capacity, model_width), gates, ups, downs, row_count
    )
    returned = lax.all_to_all(
        results.reshape(ep_count, capacity, model_width), "ep", 0, 0, tiled=True
    )
    expert_out = combined(
        returned.reshape(ep_count * capacity, model_width), slots, route_weights
    )
    return (mixer_out, expert_out)


def solution(mesh):
    return jax.shard_map(
        body,
        mesh=mesh,
        in_specs=(
            P("ep", "tp"),
            P("ep", "tp"),
            P(),
            P(),
            P(("ep", "tp"), None),
            P(),
            P(("ep", "tp"), None),
            P(("ep", "tp"), None),
            P("ep", None, "tp"),
            P("ep", None, "tp"),
            P("ep", "tp", None),
        ),
        out_specs=(P(("ep", "tp"), None), P(("ep", "tp"), None)),
        check_vma=False,
    )
```

```python
import functools

import jax
import jax.numpy as jnp
from jax import lax
from jax.experimental import pallas as pl
from jax.experimental.pallas import tpu as pltpu
from jax.sharding import PartitionSpec as P


HEAD_DIM = 64
WINDOW = 128
TOPK = 2
CHUNKS = 1
NEG_FILL = -1e30


def gathered_shards(cells, axis):
    count = lax.axis_size(axis)
    if count & (count - 1):
        return [cells] + [
            lax.ppermute(cells, axis, [(i, (i + k) % count) for i in range(count)])
            for k in range(1, count)
        ]
    shards = [cells]
    bit = count // 2
    while bit:
        perm = [(i, i ^ bit) for i in range(count)]
        shards = shards + [lax.ppermute(shard, axis, perm) for shard in shards]
        bit //= 2
    return shards


def own_rows(cells, axis):
    count = lax.axis_size(axis)
    me = lax.axis_index(axis)
    rows, width = cells.shape[0] // count, cells.shape[1]
    result = jnp.zeros((rows, count * width), cells.dtype)
    for k in range(count):
        block = lax.dynamic_slice_in_dim(cells, (me + k) % count * rows, rows, 0)
        if k:
            block = lax.ppermute(block, axis, [(i, (i + k) % count) for i in range(count)])
        source = (me - k + count) % count
        result = lax.dynamic_update_slice_in_dim(result, block, source * width, 1)
    return result


def attend_kernel(kv_heads, group, rows, seq_total, offset_ref, q_ref, before_ref, own_ref, after_ref, sink_ref, out_ref, kv_ref, vk_ref):
    step = pl.program_id(0)

    @pl.when(step == 0)
    def fill():
        place = 0
        for piece_ref in (before_ref, own_ref, after_ref):
            length = piece_ref.shape[0]
            kv_ref[place : place + length, :] = piece_ref[...]
            for kv_head in range(kv_heads):
                lanes = slice(kv_head * 2 * HEAD_DIM, (kv_head + 1) * 2 * HEAD_DIM)
                turned = pltpu.roll(piece_ref[:, lanes].astype(jnp.float32), HEAD_DIM, 1)
                vk_ref[place : place + length, lanes] = turned.astype(jnp.bfloat16)
            place += length

    span = rows + 2 * WINDOW
    first = offset_ref[0] + step * rows
    start = pl.multiple_of(step * rows, rows)
    row = lax.broadcasted_iota(jnp.int32, (rows, span), 0)
    column = lax.broadcasted_iota(jnp.int32, (rows, span), 1)
    key_pos = first - WINDOW + column
    allowed = (
        (column >= row) & (column <= row + 2 * WINDOW) & (key_pos >= 0) & (key_pos < seq_total)
    )
    lower = lax.broadcasted_iota(jnp.int32, (rows, 2 * HEAD_DIM), 1) < HEAD_DIM
    for kv_head in range(kv_heads):
        lanes = slice(kv_head * 2 * HEAD_DIM, (kv_head + 1) * 2 * HEAD_DIM)
        kv = kv_ref[pl.ds(start, span), lanes]
        vk = vk_ref[pl.ds(start, span), lanes]
        for pair in range(group // 2):
            head = kv_head * group + 2 * pair
            cols = slice(head * HEAD_DIM, (head + 2) * HEAD_DIM)
            q_pair = q_ref[:, cols] * jnp.bfloat16(HEAD_DIM ** -0.5)
            results = []
            for odd in range(2):
                q_one = jnp.where(lower != bool(odd), q_pair, jnp.zeros_like(q_pair))
                key_side, value_side = (vk, kv) if odd else (kv, vk)
                scores = lax.dot_general(
                    q_one, key_side, (((1,), (1,)), ((), ())), preferred_element_type=jnp.float32
                )
                scores = jnp.where(allowed, scores, NEG_FILL)
                sink = sink_ref[head + odd]
                top = jnp.maximum(jnp.max(scores, 1, keepdims=True), sink)
                expo = jnp.exp(scores - top)
                denom = jnp.sum(expo, 1, keepdims=True) + jnp.exp(sink - top)
                value = jnp.dot(
                    expo.astype(jnp.bfloat16), value_side, preferred_element_type=jnp.float32
                )
                results.append(value / denom)
            out_ref[:, cols] = jnp.where(lower, results[0], results[1]).astype(jnp.bfloat16)


def attend(queries, keys_values, before, after, sink_logits):
    row_count, width = queries.shape
    kv_local = keys_values.shape[1] // (2 * HEAD_DIM)
    heads = width // HEAD_DIM
    rows = 128
    offset = (lax.axis_index("ep") * row_count).astype(jnp.int32).reshape(1)
    sink_local = lax.dynamic_slice_in_dim(sink_logits, lax.axis_index("tp") * heads, heads, 0)
    seq_total = row_count * lax.axis_size("ep")
    span = rows + 2 * WINDOW
    smem = pl.BlockSpec(memory_space=pltpu.SMEM)
    pieces = (before, keys_values, after)
    wholes = [pl.BlockSpec(piece.shape, lambda i: (0, 0)) for piece in pieces]
    padded = pltpu.VMEM((row_count + 2 * WINDOW, keys_values.shape[1]), jnp.bfloat16)
    return pl.pallas_call(
        functools.partial(attend_kernel, kv_local, heads // kv_local, rows, seq_total),
        out_shape=jax.ShapeDtypeStruct(queries.shape, jnp.bfloat16),
        grid=(row_count // rows,),
        in_specs=[smem, pl.BlockSpec((rows, width), lambda i: (i, 0)), *wholes, smem],
        out_specs=pl.BlockSpec((rows, width), lambda i: (i, 0)),
        scratch_shapes=[padded, padded],
        cost_estimate=pl.CostEstimate(
            flops=8 * row_count * span * heads * HEAD_DIM,
            bytes_accessed=4 * row_count * width,
            transcendentals=row_count * span * heads,
        ),
        name="attend",
    )(offset, queries, *pieces, sink_local)


def dispatch_kernel(experts, capacity, token_ref, gain_ref, route_ref, *refs):
    out_refs, (slot_ref, normed_ref) = refs[:CHUNKS], refs[CHUNKS:]
    step = pl.program_id(0)
    count = token_ref.shape[0]

    @pl.when(step == 0)
    def first():
        rows = token_ref[...].astype(jnp.float32)
        centred = rows - jnp.mean(rows, -1, keepdims=True)
        scale = lax.rsqrt(jnp.mean(centred * centred, -1, keepdims=True) + 1e-06)
        normed_ref[...] = (centred * scale * gain_ref[...]).astype(jnp.bfloat16)
        expert = lax.broadcasted_iota(jnp.int32, (experts, count), 0)
        named = [expert == route_ref[k : k + 1, :] for k in range(TOPK)]
        member = functools.reduce(jnp.logical_or, named)
        earlier = lax.broadcasted_iota(jnp.int32, (count, count), 0) < lax.broadcasted_iota(
            jnp.int32, (count, count), 1
        )
        rank = jnp.dot(
            jnp.where(member, 1.0, 0.0).astype(jnp.bfloat16),
            jnp.where(earlier, 1.0, 0.0).astype(jnp.bfloat16),
            preferred_element_type=jnp.float32,
        ).astype(jnp.int32)
        part = capacity // CHUNKS
        chunk = sum(jnp.where(rank >= c * part, 1, 0) for c in range(1, CHUNKS))
        place = chunk * (experts * part) + expert * part + rank - chunk * part
        for k in range(TOPK):
            slot_ref[k : k + 1, :] = jnp.sum(jnp.where(named[k], place, 0), 0, keepdims=True)

    tile = out_refs[0].shape[0]
    slot = step * tile + lax.broadcasted_iota(jnp.int32, (tile, count), 0)
    hit = functools.reduce(
        jnp.logical_or, [slot == slot_ref[k : k + 1, :] for k in range(TOPK)]
    )
    rows_out = jnp.dot(
        jnp.where(hit, 1.0, 0.0).astype(jnp.bfloat16),
        normed_ref[...],
        preferred_element_type=jnp.float32,
    ).astype(jnp.bfloat16)
    for c in range(CHUNKS):

        @pl.when(step == c)
        def put():
            out_refs[c][...] = rows_out


def dispatched(tokens, gain, routes, experts, capacity):
    count, width = tokens.shape
    total = experts * capacity
    return pl.pallas_call(
        functools.partial(dispatch_kernel, experts, capacity),
        out_shape=(
            *[jax.ShapeDtypeStruct((total // CHUNKS, width), jnp.bfloat16)] * CHUNKS,
            jax.ShapeDtypeStruct((TOPK, count), jnp.int32),
        ),
        grid=(CHUNKS,),
        in_specs=[
            pl.BlockSpec((count, width), lambda i: (0, 0)),
            pl.BlockSpec((1, width), lambda i: (0, 0)),
            pl.BlockSpec((TOPK, count), lambda i: (0, 0)),
        ],
        out_specs=(
            *[pl.BlockSpec((total // CHUNKS, width), lambda i: (0, 0))] * CHUNKS,
            pl.BlockSpec((TOPK, count), lambda i: (0, 0)),
        ),
        scratch_shapes=[pltpu.VMEM((count, width), jnp.bfloat16)],
        cost_estimate=pl.CostEstimate(
            flops=2 * total * count * width, bytes_accessed=2 * (total + count) * width,
            transcendentals=count,
        ),
        name="dispatch",
    )(tokens, gain.reshape(1, width), routes.T)


def expert_kernel(shards, block, x_ref, *refs):
    weights = refs[: 3 * shards]
    out_ref, gate_s, up_s, down_s, hidden_s, sems = refs[3 * shards :]
    first = pl.program_id(0) == 0

    def copies(shard, kinds):
        part = slice(shard * block, (shard + 1) * block)
        places = (gate_s.at[:, part], up_s.at[:, part], down_s.at[part, :])
        return [
            pltpu.make_async_copy(
                weights[3 * shard + kind], places[kind], sems.at[3 * shard + kind]
            )
            for kind in kinds
        ]

    @pl.when(first)
    def start():
        for kinds in ((0, 1), (2,)):
            for shard in range(shards):
                for copy in copies(shard, kinds):
                    copy.start()

    for shard in range(shards):
        part = slice(shard * block, (shard + 1) * block)

        @pl.when(first)
        def arrive():
            for copy in copies(shard, (0, 1)):
                copy.wait()

        gate = jnp.dot(x_ref[...], gate_s[:, part], preferred_element_type=jnp.float32)
        up = jnp.dot(x_ref[...], up_s[:, part], preferred_element_type=jnp.float32)
        hidden_s[:, part] = (gate / (1.0 + jnp.exp(-gate)) * up).astype(jnp.bfloat16)

    @pl.when(first)
    def arrive_down():
        for shard in range(shards):
            copies(shard, (2,))[0].wait()

    out_ref[...] = jnp.dot(
        hidden_s[...], down_s[...], preferred_element_type=jnp.float32
    ).astype(jnp.bfloat16)


def expert_rows(rows, gates, ups, downs, tile):
    total, width = rows.shape
    shards = len(gates)
    block = gates[0].shape[1]
    hidden = shards * block
    weights = [w for group in zip(gates, ups, downs) for w in group]
    return pl.pallas_call(
        functools.partial(expert_kernel, shards, block),
        out_shape=jax.ShapeDtypeStruct(rows.shape, jnp.bfloat16),
        grid=(total // tile,),
        in_specs=[pl.BlockSpec((tile, width), lambda i: (i, 0))]
        + [pl.BlockSpec(memory_space=pl.ANY)] * len(weights),
        out_specs=pl.BlockSpec((tile, width), lambda i: (i, 0)),
        scratch_shapes=[
            pltpu.VMEM((width, hidden), jnp.bfloat16),
            pltpu.VMEM((width, hidden), jnp.bfloat16),
            pltpu.VMEM((hidden, width), jnp.bfloat16),
            pltpu.VMEM((tile, hidden), jnp.bfloat16),
            pltpu.SemaphoreType.DMA((3 * shards,)),
        ],
        compiler_params=pltpu.CompilerParams(vmem_limit_bytes=48 * 1024 * 1024),
        cost_estimate=pl.CostEstimate(
            flops=6 * total * width * hidden,
            bytes_accessed=6 * width * hidden + 4 * total * width,
            transcendentals=total * hidden,
        ),
        name="experts",
    )(rows, *weights)


def combine_kernel(slot_ref, weight_ref, *refs):
    rows_refs, (out_ref, high_ref, low_ref) = refs[:CHUNKS], refs[CHUNKS:]

    @pl.when(pl.program_id(0) == 0)
    def first():
        count, total = high_ref.shape
        slot = lax.broadcasted_iota(jnp.int32, (count, total), 1)
        mix = sum(
            jnp.where(slot == slot_ref[:, k : k + 1], weight_ref[:, k : k + 1], 0.0)
            for k in range(TOPK)
        )
        high = mix.astype(jnp.bfloat16)
        high_ref[...] = high
        low_ref[...] = (mix - high.astype(jnp.float32)).astype(jnp.bfloat16)

    total = 0.0
    for c, rows_ref in enumerate(rows_refs):
        rows = rows_ref[...]
        part = slice(c * rows.shape[0], (c + 1) * rows.shape[0])
        total += jnp.dot(high_ref[:, part], rows, preferred_element_type=jnp.float32)
        total += jnp.dot(low_ref[:, part], rows, preferred_element_type=jnp.float32)
    out_ref[...] = total.astype(jnp.bfloat16)


def combined(rows, slots, route_weights):
    part, width = rows[0].shape
    total = part * CHUNKS
    count = route_weights.shape[0]
    tile = width // 4
    return pl.pallas_call(
        combine_kernel,
        out_shape=jax.ShapeDtypeStruct((count, width), jnp.bfloat16),
        grid=(width // tile,),
        in_specs=[
            pl.BlockSpec((count, TOPK), lambda i: (0, 0)),
            pl.BlockSpec((count, TOPK), lambda i: (0, 0)),
            *[pl.BlockSpec((part, tile), lambda i: (0, i))] * CHUNKS,
        ],
        out_specs=pl.BlockSpec((count, tile), lambda i: (0, i)),
        scratch_shapes=[
            pltpu.VMEM((count, total), jnp.bfloat16),
            pltpu.VMEM((count, total), jnp.bfloat16),
        ],
        cost_estimate=pl.CostEstimate(
            flops=4 * total * count * width, bytes_accessed=2 * (total + count) * width,
            transcendentals=0,
        ),
        name="combine",
    )(slots.T, route_weights, *rows)


def body(
    queries,
    keys_values,
    sink_logits,
    out_weight,
    expert_tokens,
    norm_gain,
    routes,
    route_weights,
    gate_weight,
    up_weight,
    down_weight,
):
    ep_count = lax.axis_size("ep")
    row_count, model_width = expert_tokens.shape
    capacity = 3 * row_count * TOPK // (2 * ep_count)
    ends = ep_count - 1
    before = lax.ppermute(keys_values[-WINDOW:], "ep", [(i, i + 1) for i in range(ends)])
    after = lax.ppermute(keys_values[:WINDOW], "ep", [(i + 1, i) for i in range(ends)])
    gates = gathered_shards(gate_weight[0], "tp")
    ups = gathered_shards(up_weight[0], "tp")
    downs = gathered_shards(down_weight[0], "tp")
    *outgoing, slots = dispatched(expert_tokens, norm_gain, routes, ep_count, capacity)
    outgoing, before, after = lax.optimization_barrier((outgoing, before, after))
    part = capacity // CHUNKS
    chunk = (ep_count, part, model_width)
    arrived = [lax.all_to_all(o.reshape(chunk), "ep", 0, 0, tiled=True) for o in outgoing]
    attended = attend(queries, keys_values, before, after, sink_logits)
    token_rows = own_rows(attended, "tp")
    mixer_out = jnp.dot(token_rows, out_weight, preferred_element_type=jnp.float32).astype(
        jnp.bfloat16
    )
    returned = []
    for rows in arrived:
        rows = rows.reshape(ep_count * part, model_width)
        results = expert_rows(rows, gates, ups, downs, ep_count * part // 2)
        back = lax.all_to_all(results.reshape(chunk), "ep", 0, 0, tiled=True)
        returned.append(back.reshape(ep_count * part, model_width))
    expert_out = combined(returned, slots, route_weights)
    return (mixer_out, expert_out)


def solution(mesh):
    return jax.shard_map(
        body,
        mesh=mesh,
        in_specs=(
            P("ep", "tp"),
            P("ep", "tp"),
            P(),
            P(),
            P(("ep", "tp"), None),
            P(),
            P(("ep", "tp"), None),
            P(("ep", "tp"), None),
            P("ep", None, "tp"),
            P("ep", None, "tp"),
            P("ep", "tp", None),
        ),
        out_specs=(P(("ep", "tp"), None), P(("ep", "tp"), None)),
        check_vma=False,
    )
```
